32 devices in a mesh: kv: 8 (over z, x), tp: 4 (over y, core).
Axes of the slice: x: 2, y: 2, z: 4, core: 2. Of those that a mesh axis runs over, the one named last changes fastest.
Arguments:
- tokens: bfloat16 [64, 4, 4096], P(None, None, 'kv')
- norm_gain: float32 [4096], replicated, may hold values from 0.1 to 1.9
- w_query: bfloat16 [4096, 4096], P('kv', 'tp'), may hold values from -0.09375 to 0.09375
- w_key: bfloat16 [4096, 4096], P('kv', 'tp'), may hold values from -0.09375 to 0.09375
- w_value: bfloat16 [4096, 4096], P('kv', 'tp'), may hold values from -0.09375 to 0.09375
- w_gate: bfloat16 [4096, 4096], P('kv', 'tp'), may hold values from -0.09375 to 0.09375
- w_decay: bfloat16 [4096, 32], replicated, may hold values from -0.09375 to 0.09375
- w_beta: bfloat16 [4096, 32], replicated, may hold values from -0.09375 to 0.09375
- decay_rate: float32 [32], replicated, may hold values from 0.02 to 3
- head_gain: float32 [128], replicated, may hold values from 0.1 to 1.9
- w_out: bfloat16 [4096, 4096], P('tp', 'kv'), may hold values from -0.09375 to 0.09375
- state: float32 [64, 32, 128, 128], P('kv', 'tp'), may hold values from -0.4 to 0.4
- prev_keys: bfloat16 [64, 32, 4, 128], P('kv', 'tp'), may hold values from -6 to 6
- prev_values: bfloat16 [64, 32, 4, 128], P('kv', 'tp'), may hold values from -6 to 6
- prev_log_decay: float32 [64, 32, 4], P('kv', 'tp'), may hold values from -0.7 to -0.02
- prev_beta: float32 [64, 32, 4], P('kv', 'tp'), may hold values from 0.1 to 0.9
- accepted: int32 [64], P('kv'), may hold values from 0 to 4
Outputs:
- mixed: bfloat16 [64, 4, 4096], P('tp', None, 'kv')
- carried: float32 [64, 32, 128, 128], P('kv', 'tp')
The draws below stay inside these ranges and needn't reach their ends.
All inputs are finite; a program needn't handle non-finite values.
Results may differ from the reference program's by a relative error of at most 0.0069.
Values may be sent and summed in bfloat16 or wider, within the bound.
A program may use at most 128 MiB of HBM per device.

```python
import math
import jax
import jax.numpy as jnp
from jax import lax

D = 4096
HEADS = 32
DK = 128
DV = 128
PROPS = 4
BATCH = 64


def draw_tokens(key, part):
    column = jnp.arange(D, dtype=jnp.float32)
    rising = jnp.exp(math.log(4.0) * column / D)
    values = jax.random.normal(key, (BATCH, PROPS, D), jnp.float32) * rising
    return values.astype(jnp.bfloat16)


def place_ends(result, own_key, least, top_value):
    spot = [jax.random.randint(jax.random.fold_in(own_key, axis), (), 0, length) for axis, length in enumerate(result.shape)]
    widest = result.shape.index(max(result.shape))
    next_to = spot[:widest] + [(spot[widest] + 1) % result.shape[widest]] + spot[widest + 1:]
    return result.at[tuple(spot)].set(least).at[tuple(next_to)].set(top_value)


def block_scale(key, extent, split, low, high):
    def one(dim, parts):
        steps = jax.random.uniform(jax.random.fold_in(jax.random.fold_in(key, 6), dim), (parts,), jnp.float32, low / len(split), high / len(split))
        return jnp.repeat(jnp.exp(steps), extent[dim] // parts).reshape((-1,) + (1,) * (len(extent) - dim - 1))

    factor_of = one(*split[0])
    for cut in split[1:]:
        factor_of = factor_of * one(*cut)
    return factor_of


def scatter_about(key, extent, spread, limit, cuts=(), held_as=jnp.bfloat16):
    drawn = jax.random.normal(key, extent, jnp.float32) * spread
    if len(cuts) > 0:
        drawn = block_scale(key, extent, cuts, -0.22, 0.18) * drawn
    return jnp.clip(drawn, min=-limit, max=limit).astype(held_as)


def setup_inputs(seed: int = 0) -> dict:
    keys = jax.random.split(jax.random.key(seed), 18)
    return {
        "tokens": draw_tokens(jax.random.fold_in(keys[17], 71), 0),
        "norm_gain": jnp.clip(1.0 + 0.18 * jax.random.normal(keys[1], (D,), jnp.float32), 0.1, 1.9),
        "w_query": scatter_about(keys[2], (D, HEADS * DK), D ** -0.5, 0.09375, ((0, 8), (1, 4))),
        "w_key": scatter_about(keys[3], (D, HEADS * DK), D ** -0.5, 0.09375, ((0, 8), (1, 4))),
        "w_value": scatter_about(keys[4], (D, HEADS * DV), D ** -0.5, 0.09375, ((0, 8), (1, 4))),
        "w_gate": scatter_about(keys[5], (D, HEADS * DV), D ** -0.5, 0.09375, ((0, 8), (1, 4))),
        "w_decay": scatter_about(keys[6], (D, HEADS), D ** -0.5, 0.09375),
        "w_beta": scatter_about(keys[7], (D, HEADS), D ** -0.5, 0.09375),
        "decay_rate": jnp.clip(jnp.exp(jax.random.uniform(keys[8], (HEADS,), jnp.float32, math.log(0.02), math.log(3.0))), 0.02, 3.0),
        "head_gain": jnp.clip(1.0 + 0.18 * jax.random.normal(keys[9], (DV,), jnp.float32), 0.1, 1.9),
        "w_out": scatter_about(keys[10], (HEADS * DV, D), (HEADS * DV) ** -0.5, 0.09375, ((0, 4), (1, 8))),
        "state": scatter_about(keys[11], (BATCH, HEADS, DK, DV), 0.05, 0.4, ((0, 8), (1, 4)), jnp.float32),
        "prev_keys": scatter_about(keys[12], (BATCH, HEADS, PROPS, DK), 1.0, 6.0, ((0, 8), (1, 4))),
        "prev_values": scatter_about(keys[13], (BATCH, HEADS, PROPS, DV), 1.0, 6.0, ((0, 8), (1, 4))),
        "prev_log_decay": jnp.clip(-0.7 + 0.68 * jax.random.uniform(keys[14], (BATCH, HEADS, PROPS), jnp.float32) ** block_scale(keys[14], (BATCH, HEADS, PROPS), ((0, 8), (1, 4)), -0.2, 0.2), -0.7, -0.02),
        "prev_beta": jnp.clip(0.1 + 0.79999997 * jax.random.uniform(keys[15], (BATCH, HEADS, PROPS), jnp.float32) ** block_scale(keys[15], (BATCH, HEADS, PROPS), ((0, 8), (1, 4)), -0.2, 0.2), 0.1, 0.9),
        "accepted": place_ends(jax.random.randint(keys[16], (BATCH,), 0, PROPS + 1), jax.random.fold_in(keys[16], 1), 0, PROPS).astype(jnp.int32),
    }


epsilon = 1e-06

def unit_rows(values):
    return values * lax.rsqrt(lax.optimization_barrier(jnp.sum(values * values, axis=-1, keepdims=True)) + epsilon)

def apply_update(matrix, keyvec, valvec, logd, strength):
    decayed = jnp.exp(logd)[..., None, None] * matrix
    predicted = jnp.einsum('bhde,bhd->bhe', decayed, keyvec, precision=lax.Precision.HIGHEST)
    change = strength[..., None] * (valvec - predicted)
    return decayed + jnp.einsum('bhd,bhe->bhde', keyvec, change, precision=lax.Precision.HIGHEST)

def reference(tokens, norm_gain, w_query, w_key, w_value, w_gate, w_decay, w_beta, decay_rate, head_gain, w_out, state, prev_keys, prev_values, prev_log_decay, prev_beta, accepted):
    f32 = jnp.float32
    rowsx = tokens.astype(f32).reshape(BATCH * PROPS, D)
    scale = lax.rsqrt(lax.optimization_barrier(jnp.mean(rowsx * rowsx, axis=1, keepdims=True)) + epsilon)
    normed = (rowsx * scale * norm_gain).astype(jnp.bfloat16)
    qraw = jnp.dot(normed, w_query, preferred_element_type=f32)
    kraw = jnp.dot(normed, w_key, preferred_element_type=f32)
    vraw = jnp.dot(normed, w_value, preferred_element_type=f32)
    zraw = jnp.dot(normed, w_gate, preferred_element_type=f32)
    araw = jnp.dot(normed, w_decay, preferred_element_type=f32)
    braw = jnp.dot(normed, w_beta, preferred_element_type=f32)
    query = unit_rows(jax.nn.silu(qraw).reshape(BATCH, PROPS, HEADS, DK)) * DK ** (-0.5)
    keyrow = unit_rows(jax.nn.silu(kraw).reshape(BATCH, PROPS, HEADS, DK))
    value = jax.nn.silu(vraw).reshape(BATCH, PROPS, HEADS, DV)
    beta = jax.nn.sigmoid(braw).reshape(BATCH, PROPS, HEADS)
    logdecay = (-decay_rate * jax.nn.softplus(araw)).reshape(BATCH, PROPS, HEADS)
    old_keys = unit_rows(prev_keys.astype(f32))
    old_values = prev_values.astype(f32)
    matrix = state
    for proposal in range(PROPS):
        keep = (proposal < accepted).astype(f32)[:, None]
        matrix = apply_update(matrix, old_keys[:, :, proposal], old_values[:, :, proposal], prev_log_decay[:, :, proposal] * keep, prev_beta[:, :, proposal] * keep)
    carried = matrix
    results = []
    for proposal in range(PROPS):
        matrix = apply_update(matrix, keyrow[:, proposal], value[:, proposal], logdecay[:, proposal], beta[:, proposal])
        results.append(jnp.einsum('bhde,bhd->bhe', matrix, query[:, proposal], precision=lax.Precision.HIGHEST))
    attended = jnp.stack(results, axis=1)
    zgate = zraw.reshape(BATCH, PROPS, HEADS, DV)
    headout = attended * lax.rsqrt(lax.optimization_barrier(jnp.mean(attended * attended, axis=-1, keepdims=True)) + epsilon)
    headout = (headout * head_gain * jax.nn.silu(zgate)).astype(jnp.bfloat16).reshape(BATCH * PROPS, HEADS * DV)
    mixed = jnp.dot(headout, w_out, preferred_element_type=f32).astype(jnp.bfloat16)
    return (mixed.reshape(BATCH, PROPS, D), carried)
```

```python
import functools

import jax
import jax.numpy as jnp
from jax import lax
from jax.experimental import pallas as pl
from jax.experimental.pallas import tpu as pltpu
from jax.sharding import PartitionSpec as P

epsilon = 1e-06
MESH = pl.DeviceIdType.MESH
f32 = jnp.float32
bf16 = jnp.bfloat16
HIGH = lax.Precision.HIGHEST


def exact_dot(a, b, dims=((1,), (0,))):
    return lax.dot_general(a, b, (dims, ((), ())), precision=HIGH, preferred_element_type=f32)


def fast_dot(a, b, dims=((1,), (0,))):
    return lax.dot_general(a, b, (dims, ((), ())), preferred_element_type=f32)


def split(a):
    high = a.astype(bf16)
    return high, (a - high.astype(f32)).astype(bf16)


def split_dot(a, b, dims=((1,), (0,))):
    ah, al = split(a)
    bh, bl = split(b)
    return fast_dot(ah, bh, dims) + (fast_dot(ah, bl, dims) + fast_dot(al, bh, dims))


def grid_ids(rows, props):
    r = lax.broadcasted_iota(jnp.int32, (rows, rows), 0)
    c = lax.broadcasted_iota(jnp.int32, (rows, rows), 1)
    return r, c, (r // props) == (c // props)


def chain(g, beta, key, props):
    rows = key.shape[0]
    r, c, same = grid_ids(rows, props)
    lower = same & (c <= r)
    g_row = jnp.sum(jnp.where(r == c, g, 0.0), axis=0, keepdims=True)
    cum = jnp.sum(jnp.where(lower, g_row, 0.0), axis=1, keepdims=True)
    cum_row = jnp.sum(jnp.where(same & (r <= c), g, 0.0), axis=0, keepdims=True)
    decay = jnp.where(lower, jnp.exp(jnp.where(lower, cum - cum_row, 0.0)), 0.0)
    after = jnp.sum(jnp.where(same & (c > r), g_row, 0.0), axis=1, keepdims=True)
    return cum, decay, after, same & (c < r)


def solve(a, rhs, props):
    power, factors, reach = a, [], 2
    while reach < props:
        power = split_dot(power, power)
        factors.append(power)
        reach *= 2
    for factor in factors[::-1]:
        rhs = rhs + split_dot(factor, rhs)
    return rhs - split_dot(a, rhs)


def spread_rows(x, groups, props):
    owner = lax.broadcasted_iota(jnp.int32, x.shape, 0)
    owner = (owner // props) % groups
    return jnp.concatenate([jnp.where(owner == i, x, jnp.zeros_like(x)) for i in range(groups)], axis=1)


def carried_kernel(state_ref, keys_ref, values_ref, logd_ref, beta_ref, acc_ref, out_ref, krow, vrow):
    seqs, heads, dk, dv = state_ref.shape
    props = keys_ref.shape[2]
    rows = heads * props
    first = pl.program_id(0) * seqs
    row4 = lax.broadcasted_iota(jnp.int32, (rows, props), 0)
    lane4 = lax.broadcasted_iota(jnp.int32, (rows, props), 1)
    pick = (row4 % props) == lane4
    rowh = lax.broadcasted_iota(jnp.int32, (rows, heads), 0)
    laneh = lax.broadcasted_iota(jnp.int32, (rows, heads), 1)
    repeat = jnp.where((rowh // props) == laneh, 1.0, 0.0)
    prop_of = lax.broadcasted_iota(jnp.int32, (rows, 1), 0) % props
    for s in range(seqs):
        for h in range(heads):
            krow[s, h * props : (h + 1) * props, :] = keys_ref[s, h].astype(f32)
            vrow[s, h * props : (h + 1) * props, :] = values_ref[s, h].astype(f32)
    for s in range(seqs):
        keep = prop_of < acc_ref[first + s]
        g = jnp.sum(jnp.where(pick, exact_dot(repeat, logd_ref[s]), 0.0), axis=1, keepdims=True)
        b = jnp.sum(jnp.where(pick, exact_dot(repeat, beta_ref[s]), 0.0), axis=1, keepdims=True)
        g = jnp.where(keep, g, 0.0)
        b = jnp.where(keep, b, 0.0)
        key = krow[s]
        key = key * lax.rsqrt(jnp.sum(key * key, axis=1, keepdims=True) + epsilon)
        value = vrow[s]
        cum, decay, after, strict = chain(g, b, key, props)
        kh, kl = split(key)
        kk = split_dot(key, key, ((1,), (1,)))
        a = jnp.where(strict, b * decay * kk, 0.0)
        st = state_ref[s].reshape(heads * dk, dv)
        both = jnp.concatenate([kh, kl], axis=0)
        seen = fast_dot(spread_rows(both, heads, props), st.astype(bf16))
        seen = seen[:rows] + seen[rows:]
        u = solve(a, b * (value - jnp.exp(cum) * seen), props) * jnp.exp(after)
        uh, ul = split(u)
        left = spread_rows(jnp.concatenate([kh, kl, kh], axis=0), heads, props)
        right = jnp.concatenate([uh, uh, ul], axis=0)
        change = fast_dot(left, right, ((0,), (0,)))
        total = jnp.exp(cum + after)
        for h in range(heads):
            out_ref[s, h] = total[h * props : h * props + 1, :] * state_ref[s, h] + change[h * dk : (h + 1) * dk]


def carried_call(state, prev_keys, prev_values, prev_log_decay, prev_beta, accepted):
    seqs, heads, dk, dv = state.shape
    props = prev_keys.shape[2]
    step = 2 if seqs % 2 == 0 else 1
    at4 = lambda i: (i, 0, 0, 0)
    at3 = lambda i: (i, 0, 0)
    return pl.pallas_call(
        carried_kernel,
        grid=(seqs // step,),
        out_shape=jax.ShapeDtypeStruct(state.shape, f32),
        in_specs=[
            pl.BlockSpec((step, heads, dk, dv), at4),
            pl.BlockSpec((step, heads, props, dk), at4),
            pl.BlockSpec((step, heads, props, dv), at4),
            pl.BlockSpec((step, heads, props), at3),
            pl.BlockSpec((step, heads, props), at3),
            pl.BlockSpec(memory_space=pltpu.SMEM),
        ],
        out_specs=pl.BlockSpec((step, heads, dk, dv), at4),
        scratch_shapes=[pltpu.VMEM((step, heads * props, dk), f32), pltpu.VMEM((step, heads * props, dv), f32)],
        cost_estimate=pl.CostEstimate(flops=2 * state.size * props, bytes_accessed=8 * state.size, transcendentals=0),
    )(state, prev_keys, prev_values, prev_log_decay, prev_beta, accepted)


def step_kernel(
    nx, nz, ntp,
    tok_ref, gain_ref, wd_hbm, wb_hbm, rate_ref, hgain_ref, wq_hbm, wk_hbm, wv_hbm, wz_hbm, wo_hbm, car_hbm,
    out_ref,
    xrow, w_v, wo_v, wd_v, wb_v, car_v, ssb, nb, xs, xr, own, zs, zr, axs, axr, aown, azs, azr, abt, gat, terms, ts, tr,
    loc, ss_s, ss_r, x_s, x_r, z_s, z_r, gz_s, gz_r, gx_s, gx_r, t_s, t_r,
):
    nkv = nx * nz
    me = lax.axis_index("kv")
    tp = lax.axis_index("tp")
    z_me, x_me = me // nx, me % nx
    width, rs = nb.shape[3], nb.shape[2]
    heads = xs.shape[0]
    dk = hgain_ref.shape[1]
    seqs_all, props = tok_ref.shape[0], tok_ref.shape[1]
    rows_all = seqs_all * props
    seqs = car_v.shape[0]
    nheads = wd_v.shape[1]
    dmodel = width * nkv

    loads = [
        pltpu.make_async_copy(src, w_v.at[i], loc.at[i]) for i, src in enumerate((wq_hbm, wk_hbm, wv_hbm, wz_hbm))
    ]
    mine = pl.ds(pl.multiple_of(me * width, width), width)
    loads.append(pltpu.make_async_copy(wd_hbm.at[mine], wd_v, loc.at[4]))
    loads.append(pltpu.make_async_copy(wb_hbm.at[mine], wb_v, loc.at[5]))
    late = [pltpu.make_async_copy(car_hbm, car_v, loc.at[6]), pltpu.make_async_copy(wo_hbm, wo_v, loc.at[7])]
    for load in loads + late:
        load.start()

    barrier = pltpu.get_barrier_semaphore()
    for r in range(1, nkv):
        pl.semaphore_signal(barrier, inc=1, device_id={"kv": lax.rem(me + r, nkv)}, device_id_type=MESH)
    for r in range(1, ntp):
        pl.semaphore_signal(barrier, inc=1, device_id={"tp": lax.rem(tp + r, ntp)}, device_id_type=MESH)

    for s in range(seqs_all):
        xrow[s * props : (s + 1) * props, :] = tok_ref[s].astype(f32)
    for d in range(nkv):
        part = xrow[d * rs : (d + 1) * rs, :]
        sq = jnp.sum(part * part, axis=1, keepdims=True)
        eye = lax.broadcasted_iota(jnp.int32, (rs, rs), 0) == lax.broadcasted_iota(jnp.int32, (rs, rs), 1)
        ssb[me, d : d + 1, 0:rs] = jnp.sum(jnp.where(eye, sq, 0.0), axis=0, keepdims=True)
    pl.semaphore_wait(barrier, nkv - 1 + ntp - 1)

    def kv_copy(src, dst, send, recv, kv):
        return pltpu.make_async_remote_copy(
            src_ref=src, dst_ref=dst, send_sem=send, recv_sem=recv, device_id={"kv": kv}, device_id_type=MESH
        )

    def ss_copy(r, slot):
        return kv_copy(ssb.at[me], ssb.at[slot], ss_s.at[r - 1], ss_r.at[r - 1], lax.rem(me + r, nkv))

    for r in range(1, nkv):
        ss_copy(r, me).start()
    for r in range(1, nkv):
        ss_copy(r, lax.rem(me - r + nkv, nkv)).wait_recv()
    total_sq = ssb[0]
    for d in range(1, nkv):
        total_sq = total_sq + ssb[d]
    gain = gain_ref[:, mine]
    for d in range(nkv):
        eye = lax.broadcasted_iota(jnp.int32, (rs, rs), 0) == lax.broadcasted_iota(jnp.int32, (rs, rs), 1)
        col = jnp.sum(jnp.where(eye, total_sq[d : d + 1, 0:rs], 0.0), axis=1, keepdims=True)
        scale = lax.rsqrt(col / dmodel + epsilon)
        nb[d // nx, d % nx] = (xrow[d * rs : (d + 1) * rs, :] * scale * gain).astype(bf16)
    for load in loads:
        load.wait()

    def x_copy(h, r):
        return kv_copy(xs.at[h, r - 1], xr.at[h, r - 1], x_s.at[h, r - 1], x_r.at[h, r - 1], z_me * nx + lax.rem(x_me + r, nx))

    def ax_copy(r):
        return kv_copy(axs.at[r - 1], axr.at[r - 1], x_s.at[heads, r - 1], x_r.at[heads, r - 1], z_me * nx + lax.rem(x_me + r, nx))

    def z_copy(h, r):
        to = lax.rem(z_me + r, nz)
        return kv_copy(zs.at[h, to], zr.at[h, r - 1], z_s.at[h, r - 1], z_r.at[h, r - 1], to * nx + x_me)

    def az_copy(r):
        to = lax.rem(z_me + r, nz)
        return kv_copy(azs.at[to], azr.at[r - 1], z_s.at[heads, r - 1], z_r.at[heads, r - 1], to * nx + x_me)

    def lanes(h):
        return pl.ds(pl.multiple_of(h * dk, dk), dk)

    def gz_copy(h, r, slot):
        here = gat.at[z_me, x_me, :, lanes(h)]
        there = gat.at[slot, x_me, :, lanes(h)]
        return kv_copy(here, there, gz_s.at[h, r - 1], gz_r.at[h, r - 1], lax.rem(z_me + r, nz) * nx + x_me)

    def gx_copy(h, r, slot):
        here = gat.at[:, x_me, :, lanes(h)]
        there = gat.at[:, slot, :, lanes(h)]
        return kv_copy(here, there, gx_s.at[h, r - 1], gx_r.at[h, r - 1], z_me * nx + lax.rem(x_me + r, nx))

    wab = jnp.concatenate([wd_v[...], wb_v[...], jnp.zeros((width, axs.shape[3] - 2 * nheads), bf16)], axis=1)
    for r in range(nx):
        rows = nb[:, lax.rem(x_me + r, nx)].reshape(nz * rs, width)
        got = fast_dot(rows, wab).reshape(nz, rs, -1)
        if r == 0:
            aown[...] = got
        else:
            axs[r - 1] = got.astype(bf16)
            ax_copy(r).start()

    @pl.loop(0, heads)
    def project(h):
        for r in list(range(1, nx)) + [0]:
            rows = nb[:, lax.rem(x_me + r, nx)].reshape(nz * rs, width)
            for i in range(4):
                got = fast_dot(rows, w_v[i, :, lanes(h)]).reshape(nz, rs, dk)
                at = slice(i * dk, (i + 1) * dk)
                if r == 0:
                    own[h, :, :, at] = got
                else:
                    xs[h, r - 1, :, :, at] = got.astype(bf16)
            if r > 0:
                x_copy(h, r).start()

    for r in range(1, nx):
        ax_copy(r).wait_recv()
        aown[...] += axr[r - 1].astype(f32)
    azs[...] = aown[...].astype(bf16)
    for r in range(1, nz):
        az_copy(r).start()

    late[0].wait()

    def stage_b(h):
        for r in range(1, nx):
            x_copy(h, r).wait_recv()
        pair = own[h]
        for r in range(1, nx):
            pair = pair + xr[h, r - 1].astype(f32)
        zs[h] = pair.astype(bf16)
        own[h] = pair
        for r in range(1, nz):
            z_copy(h, r).start()

    def stage_c(h):
        for r in range(1, nz):
            z_copy(h, r).wait_recv()
        tot = own[h, z_me]
        for r in range(1, nz):
            tot = tot + zr[h, r - 1].astype(f32)
        qraw, kraw, vraw, zraw = (tot[:, i * dk : (i + 1) * dk] for i in range(4))

        def unit(v):
            v = v * jax.nn.sigmoid(v)
            return v * lax.rsqrt(jnp.sum(v * v, axis=1, keepdims=True) + epsilon)

        query = unit(qraw) * dk ** (-0.5)
        key = unit(kraw)
        value = vraw * jax.nn.sigmoid(vraw)
        ab = abt[...]
        lane = lax.broadcasted_iota(jnp.int32, ab.shape, 1)
        head = tp * heads + h
        araw = jnp.sum(jnp.where(lane == head, ab, 0.0), axis=1, keepdims=True)
        braw = jnp.sum(jnp.where(lane == head + nheads, ab, 0.0), axis=1, keepdims=True)
        rate_lane = lax.broadcasted_iota(jnp.int32, rate_ref.shape, 1)
        rate = jnp.sum(jnp.where(rate_lane == head, rate_ref[...], 0.0), axis=1, keepdims=True)
        beta = jax.nn.sigmoid(braw)
        softplus = jnp.maximum(araw, 0.0) + jnp.log(1.0 + jnp.exp(-jnp.abs(araw)))
        g = -rate * softplus
        cum, decay, _, strict = chain(g, beta, key, props)
        x = jnp.concatenate([key, query], axis=0)
        prods = split_dot(x, key, ((1,), (1,)))
        a = jnp.where(strict, beta * decay * prods[:rs], 0.0)
        xh, xl = split(x)
        st = car_v[:, h].reshape(seqs * dk, -1)
        sh, sl = split(st)
        wide = spread_rows(xh, seqs, props)
        seen = fast_dot(wide, sh) + (fast_dot(spread_rows(xl, seqs, props), sh) + fast_dot(wide, sl))
        grow = jnp.exp(cum)
        u = solve(a, beta * (value - grow * seen[:rs]), props)
        att = grow * seen[rs:] + split_dot(decay * prods[rs:], u)
        ho = att * lax.rsqrt(jnp.mean(att * att, axis=1, keepdims=True) + epsilon)
        ho = ho * hgain_ref[...] * (zraw * jax.nn.sigmoid(zraw))
        gat[z_me, x_me, :, lanes(h)] = ho.astype(bf16)
        for r in range(1, nz):
            gz_copy(h, r, z_me).start()

    def stage_d(h):
        for r in range(1, nz):
            gz_copy(h, r, lax.rem(z_me - r + nz, nz)).wait_recv()
        for r in range(1, nx):
            gx_copy(h, r, x_me).start()

    lag_c, lag_d = 1, 2
    stage_b(0)
    for r in range(1, nz):
        az_copy(r).wait_recv()
    ab_total = aown[z_me]
    for r in range(1, nz):
        ab_total = ab_total + azr[r - 1].astype(f32)
    abt[...] = ab_total

    @pl.loop(1, heads + lag_d)
    def pipeline(i):
        @pl.when(i < heads)
        def _():
            stage_b(i)

        @pl.when((i >= lag_c) & (i < heads + lag_c))
        def _():
            stage_c(i - lag_c)

        @pl.when(i >= lag_d)
        def _():
            stage_d(i - lag_d)

    late[1].wait()

    @pl.loop(0, heads)
    def arrived(h):
        for r in range(1, nx):
            gx_copy(h, r, lax.rem(x_me - r + nx, nx)).wait_recv()

    share = rows_all // ntp

    def t_copy(r):
        to = lax.rem(tp + r, ntp)
        return pltpu.make_async_remote_copy(
            src_ref=ts.at[to], dst_ref=tr.at[r - 1], send_sem=t_s.at[r - 1], recv_sem=t_r.at[r - 1],
            device_id={"tp": to}, device_id_type=MESH,
        )

    got = fast_dot(gat[...].reshape(rows_all, -1), wo_v[...]).reshape(ntp, share, -1)
    terms[...] = got
    ts[...] = got.astype(bf16)
    for r in range(1, ntp):
        t_copy(r).start()
    for r in range(1, ntp):
        t_copy(r).wait_recv()
    result = terms[tp]
    for r in range(1, ntp):
        result = result + tr[r - 1].astype(f32)
    out_ref[...] = result.astype(bf16)

    for r in range(1, nkv):
        ss_copy(r, me).wait_send()
    for r in range(1, nx):
        ax_copy(r).wait_send()
    for r in range(1, nz):
        az_copy(r).wait_send()
    for r in range(1, ntp):
        t_copy(r).wait_send()

    @pl.loop(0, heads)
    def drain(h):
        for r in range(1, nx):
            x_copy(h, r).wait_send()
            gx_copy(h, r, x_me).wait_send()
        for r in range(1, nz):
            z_copy(h, r).wait_send()
            gz_copy(h, r, z_me).wait_send()


def step_call(nkv, ntp, tokens, norm_gain, wd, wb, rate, hgain, wq, wk, wv, wz, wo, carried):
    nx = 1
    while nx * nx * 4 <= nkv:
        nx *= 2
    nz = nkv // nx
    seqs, heads, dk, dv = carried.shape
    seqs_all, props, width = tokens.shape
    rs = seqs * props
    rows_all = seqs_all * props
    nheads = wd.shape[1]
    ab = -(-2 * nheads // 128) * 128
    out_cols = wo.shape[1]
    share = rows_all // ntp
    vmem = pl.BlockSpec(memory_space=pltpu.VMEM)
    anyw = pl.BlockSpec(memory_space=pl.ANY)
    V = pltpu.VMEM
    dma = pltpu.SemaphoreType.DMA
    return pl.pallas_call(
        functools.partial(step_kernel, nx, nz, ntp),
        out_shape=jax.ShapeDtypeStruct((share, out_cols), bf16),
        in_specs=[vmem, vmem, anyw, anyw, vmem, vmem] + [anyw] * 6,
        out_specs=vmem,
        scratch_shapes=[
            V((rows_all, width), f32),
            V((4,) + wq.shape, bf16),
            V(wo.shape, bf16),
            V((width, nheads), bf16),
            V((width, nheads), bf16),
            V(carried.shape, f32),
            V((nkv, nkv, 128), f32),
            V((nz, nx, rs, width), bf16),
            V((heads, nx - 1, nz, rs, 4 * dk), bf16),
            V((heads, nx - 1, nz, rs, 4 * dk), bf16),
            V((heads, nz, rs, 4 * dk), f32),
            V((heads, nz, rs, 4 * dk), bf16),
            V((heads, nz - 1, rs, 4 * dk), bf16),
            V((nx - 1, nz, rs, ab), bf16),
            V((nx - 1, nz, rs, ab), bf16),
            V((nz, rs, ab), f32),
            V((nz, rs, ab), bf16),
            V((nz - 1, rs, ab), bf16),
            V((rs, ab), f32),
            V((nz, nx, rs, heads * dv), bf16),
            V((ntp, share, out_cols), f32),
            V((ntp, share, out_cols), bf16),
            V((ntp - 1, share, out_cols), bf16),
            dma((8,)),
            dma((nkv - 1,)), dma((nkv - 1,)),
            dma((heads + 1, nx - 1)), dma((heads + 1, nx - 1)),
            dma((heads + 1, nz - 1)), dma((heads + 1, nz - 1)),
            dma((heads, nz - 1)), dma((heads, nz - 1)),
            dma((heads, nx - 1)), dma((heads, nx - 1)),
            dma((ntp - 1,)), dma((ntp - 1,)),
        ],
        compiler_params=pltpu.CompilerParams(
            collective_id=0, has_side_effects=True, vmem_limit_bytes=48 * 1024 * 1024
        ),
    )(tokens, norm_gain, wd, wb, rate, hgain, wq, wk, wv, wz, wo, carried)


def solution(mesh):
    nkv, ntp = mesh.shape["kv"], mesh.shape["tp"]

    def per_device(
        tokens, norm_gain, w_query, w_key, w_value, w_gate, w_decay, w_beta, decay_rate, head_gain, w_out,
        state, prev_keys, prev_values, prev_log_decay, prev_beta, accepted,
    ):
        carried = carried_call(state, prev_keys, prev_values, prev_log_decay, prev_beta, accepted)
        mixed = step_call(
            nkv, ntp, tokens, norm_gain.reshape(1, -1), w_decay, w_beta, decay_rate.reshape(1, -1),
            head_gain.reshape(1, -1), w_query, w_key, w_value, w_gate, w_out, carried,
        )
        return mixed.reshape(-1, tokens.shape[1], mixed.shape[1]), carried

    placed = (
        P(None, None, "kv"), P(), P("kv", "tp"), P("kv", "tp"), P("kv", "tp"), P("kv", "tp"), P(), P(), P(), P(),
        P("tp", "kv"), P("kv", "tp", None, None), P("kv", "tp", None, None), P("kv", "tp", None, None),
        P("kv", "tp", None), P("kv", "tp", None), P("kv"),
    )
    return jax.shard_map(
        per_device,
        mesh=mesh,
        in_specs=placed,
        out_specs=(P("tp", None, "kv"), P("kv", "tp", None, None)),
        check_vma=False,
    )
```

```python
import functools

import jax
import jax.numpy as jnp
from jax import lax
from jax.experimental import pallas as pl
from jax.experimental.pallas import tpu as pltpu
from jax.sharding import PartitionSpec as P

epsilon = 1e-06
MESH = pl.DeviceIdType.MESH
f32 = jnp.float32
bf16 = jnp.bfloat16
HIGH = lax.Precision.HIGHEST


def exact_dot(a, b, dims=((1,), (0,))):
    return lax.dot_general(a, b, (dims, ((), ())), precision=HIGH, preferred_element_type=f32)


def fast_dot(a, b, dims=((1,), (0,))):
    return lax.dot_general(a, b, (dims, ((), ())), preferred_element_type=f32)


def split(a):
    high = a.astype(bf16)
    return high, (a - high.astype(f32)).astype(bf16)


def split_dot(a, b, dims=((1,), (0,))):
    ah, al = split(a)
    bh, bl = split(b)
    return fast_dot(ah, bh, dims) + (fast_dot(ah, bl, dims) + fast_dot(al, bh, dims))


def grid_ids(rows, props):
    r = lax.broadcasted_iota(jnp.int32, (rows, rows), 0)
    c = lax.broadcasted_iota(jnp.int32, (rows, rows), 1)
    return r, c, (r // props) == (c // props)


def chain(g, beta, key, props):
    rows = key.shape[0]
    r, c, same = grid_ids(rows, props)
    lower = same & (c <= r)
    g_row = jnp.sum(jnp.where(r == c, g, 0.0), axis=0, keepdims=True)
    cum = jnp.sum(jnp.where(lower, g_row, 0.0), axis=1, keepdims=True)
    cum_row = jnp.sum(jnp.where(same & (r <= c), g, 0.0), axis=0, keepdims=True)
    decay = jnp.where(lower, jnp.exp(jnp.where(lower, cum - cum_row, 0.0)), 0.0)
    after = jnp.sum(jnp.where(same & (c > r), g_row, 0.0), axis=1, keepdims=True)
    return cum, decay, after, same & (c < r)


def solve(a, rhs, props):
    power, factors, reach = a, [], 2
    while reach < props:
        power = split_dot(power, power)
        factors.append(power)
        reach *= 2
    for factor in factors[::-1]:
        rhs = rhs + split_dot(factor, rhs)
    return rhs - split_dot(a, rhs)


def spread_rows(x, groups, props):
    owner = lax.broadcasted_iota(jnp.int32, x.shape, 0)
    owner = (owner // props) % groups
    return jnp.concatenate([jnp.where(owner == i, x, jnp.zeros_like(x)) for i in range(groups)], axis=1)


def carried_kernel(state_ref, keys_ref, values_ref, logd_ref, beta_ref, acc_ref, out_ref, krow, vrow):
    seqs, heads, dk, dv = state_ref.shape
    props = keys_ref.shape[2]
    rows = heads * props
    first = pl.program_id(0) * seqs
    row4 = lax.broadcasted_iota(jnp.int32, (rows, props), 0)
    lane4 = lax.broadcasted_iota(jnp.int32, (rows, props), 1)
    pick = (row4 % props) == lane4
    rowh = lax.broadcasted_iota(jnp.int32, (rows, heads), 0)
    laneh = lax.broadcasted_iota(jnp.int32, (rows, heads), 1)
    repeat = jnp.where((rowh // props) == laneh, 1.0, 0.0)
    prop_of = lax.broadcasted_iota(jnp.int32, (rows, 1), 0) % props
    for s in range(seqs):
        for h in range(heads):
            krow[s, h * props : (h + 1) * props, :] = keys_ref[s, h].astype(f32)
            vrow[s, h * props : (h + 1) * props, :] = values_ref[s, h].astype(f32)
    for s in range(seqs):
        keep = prop_of < acc_ref[first + s]
        g = jnp.sum(jnp.where(pick, exact_dot(repeat, logd_ref[s], ((1,), (1,))), 0.0), axis=1, keepdims=True)
        b = jnp.sum(jnp.where(pick, exact_dot(repeat, beta_ref[s], ((1,), (1,))), 0.0), axis=1, keepdims=True)
        g = jnp.where(keep, g, 0.0)
        b = jnp.where(keep, b, 0.0)
        key = krow[s]
        key = key * lax.rsqrt(jnp.sum(key * key, axis=1, keepdims=True) + epsilon)
        value = vrow[s]
        cum, decay, after, strict = chain(g, b, key, props)
        kh, kl = split(key)
        kk = split_dot(key, key, ((1,), (1,)))
        a = jnp.where(strict, b * decay * kk, 0.0)
        st = state_ref[s].reshape(heads * dk, dv)
        both = jnp.concatenate([kh, kl], axis=0)
        seen = fast_dot(spread_rows(both, heads, props), st.astype(bf16))
        seen = seen[:rows] + seen[rows:]
        u = solve(a, b * (value - jnp.exp(cum) * seen), props) * jnp.exp(after)
        uh, ul = split(u)
        left = spread_rows(jnp.concatenate([kh, kl, kh], axis=0), heads, props)
        right = jnp.concatenate([uh, uh, ul], axis=0)
        change = fast_dot(left, right, ((0,), (0,)))
        total = jnp.exp(cum + after)
        for h in range(heads):
            out_ref[s, h] = total[h * props : h * props + 1, :] * state_ref[s, h] + change[h * dk : (h + 1) * dk]


def carried_call(state, prev_keys, prev_values, prev_log_decay, prev_beta, accepted):
    seqs, heads, dk, dv = state.shape
    props = prev_keys.shape[2]
    step = 4 if seqs % 4 == 0 else 1
    at4 = lambda i: (i, 0, 0, 0)
    at3 = lambda i: (i, 0, 0)
    return pl.pallas_call(
        carried_kernel,
        grid=(seqs // step,),
        out_shape=jax.ShapeDtypeStruct(state.shape, f32),
        in_specs=[
            pl.BlockSpec((step, heads, dk, dv), at4),
            pl.BlockSpec((step, heads, props, dk), at4),
            pl.BlockSpec((step, heads, props, dv), at4),
            pl.BlockSpec((step, props, heads), at3),
            pl.BlockSpec((step, props, heads), at3),
            pl.BlockSpec(memory_space=pltpu.SMEM),
        ],
        out_specs=pl.BlockSpec((step, heads, dk, dv), at4),
        scratch_shapes=[pltpu.VMEM((step, heads * props, dk), f32), pltpu.VMEM((step, heads * props, dv), f32)],
        cost_estimate=pl.CostEstimate(flops=2 * state.size * props, bytes_accessed=8 * state.size, transcendentals=0),
    )(state, prev_keys, prev_values, prev_log_decay, prev_beta, accepted)


def step_kernel(
    nx, nz, ntp,
    tok_ref, gain_ref, wd_hbm, wb_hbm, rate_ref, hgain_ref, wq_hbm, wk_hbm, wv_hbm, wz_hbm, wo_hbm, car_hbm,
    out_ref,
    xrow, w_v, wo_v, wd_v, wb_v, car_v, ssb, nb, xs, xr, own, zs, zr, axs, axr, aown, azs, azr, abt, gat, terms, ts, tr,
    loc, ss_s, ss_r, x_s, x_r, z_s, z_r, gz_s, gz_r, gx_s, gx_r, t_s, t_r,
):
    nkv = nx * nz
    me = lax.axis_index("kv")
    tp = lax.axis_index("tp")
    z_me, x_me = me // nx, me % nx
    width, rs = nb.shape[3], nb.shape[2]
    heads = xs.shape[0]
    dk = hgain_ref.shape[1]
    seqs_all, props = tok_ref.shape[0], tok_ref.shape[1]
    rows_all = seqs_all * props
    seqs = car_v.shape[0]
    nheads = wd_v.shape[0]
    dmodel = width * nkv

    loads = [
        pltpu.make_async_copy(src, w_v.at[i], loc.at[i]) for i, src in enumerate((wq_hbm, wk_hbm, wv_hbm, wz_hbm))
    ]
    mine = pl.ds(pl.multiple_of(me * width, width), width)
    loads.append(pltpu.make_async_copy(wd_hbm.at[:, mine], wd_v, loc.at[4]))
    loads.append(pltpu.make_async_copy(wb_hbm.at[:, mine], wb_v, loc.at[5]))
    late = [pltpu.make_async_copy(car_hbm, car_v, loc.at[6]), pltpu.make_async_copy(wo_hbm, wo_v, loc.at[7])]
    for load in loads:
        load.start()

    barrier = pltpu.get_barrier_semaphore()
    for r in range(1, nkv):
        pl.semaphore_signal(barrier, inc=1, device_id={"kv": lax.rem(me + r, nkv)}, device_id_type=MESH)
    for r in range(1, ntp):
        pl.semaphore_signal(barrier, inc=1, device_id={"tp": lax.rem(tp + r, ntp)}, device_id_type=MESH)

    for s in range(seqs_all):
        xrow[s * props : (s + 1) * props, :] = tok_ref[s].astype(f32)
    for d in range(nkv):
        part = xrow[d * rs : (d + 1) * rs, :]
        sq = jnp.sum(part * part, axis=1, keepdims=True)
        eye = lax.broadcasted_iota(jnp.int32, (rs, rs), 0) == lax.broadcasted_iota(jnp.int32, (rs, rs), 1)
        ssb[me, d : d + 1, 0:rs] = jnp.sum(jnp.where(eye, sq, 0.0), axis=0, keepdims=True)
    pl.semaphore_wait(barrier, nkv - 1 + ntp - 1)

    def kv_copy(src, dst, send, recv, kv):
        return pltpu.make_async_remote_copy(
            src_ref=src, dst_ref=dst, send_sem=send, recv_sem=recv, device_id={"kv": kv}, device_id_type=MESH
        )

    def ss_copy(r, slot):
        return kv_copy(ssb.at[me], ssb.at[slot], ss_s.at[r - 1], ss_r.at[r - 1], lax.rem(me + r, nkv))

    for r in range(1, nkv):
        ss_copy(r, me).start()
    for r in range(1, nkv):
        ss_copy(r, lax.rem(me - r + nkv, nkv)).wait_recv()
    total_sq = ssb[0]
    for d in range(1, nkv):
        total_sq = total_sq + ssb[d]
    gain = gain_ref[:, mine]
    for d in range(nkv):
        eye = lax.broadcasted_iota(jnp.int32, (rs, rs), 0) == lax.broadcasted_iota(jnp.int32, (rs, rs), 1)
        col = jnp.sum(jnp.where(eye, total_sq[d : d + 1, 0:rs], 0.0), axis=1, keepdims=True)
        scale = lax.rsqrt(col / dmodel + epsilon)
        nb[d // nx, d % nx] = (xrow[d * rs : (d + 1) * rs, :] * scale * gain).astype(bf16)
    for load in loads:
        load.wait()
    for load in late:
        load.start()

    def x_copy(h, r):
        return kv_copy(xs.at[h, r - 1], xr.at[h, r - 1], x_s.at[h, r - 1], x_r.at[h, r - 1], z_me * nx + lax.rem(x_me + r, nx))

    def ax_copy(r):
        return kv_copy(axs.at[r - 1], axr.at[r - 1], x_s.at[heads, r - 1], x_r.at[heads, r - 1], z_me * nx + lax.rem(x_me + r, nx))

    def z_copy(h, r):
        to = lax.rem(z_me + r, nz)
        return kv_copy(zs.at[h, to], zr.at[h, r - 1], z_s.at[h, r - 1], z_r.at[h, r - 1], to * nx + x_me)

    def az_copy(r):
        to = lax.rem(z_me + r, nz)
        return kv_copy(azs.at[to], azr.at[r - 1], z_s.at[heads, r - 1], z_r.at[heads, r - 1], to * nx + x_me)

    def lanes(h):
        return pl.ds(pl.multiple_of(h * dk, dk), dk)

    def gz_copy(h, r, slot):
        here = gat.at[h, x_me, z_me]
        there = gat.at[h, x_me, slot]
        return kv_copy(here, there, gz_s.at[h, r - 1], gz_r.at[h, r - 1], lax.rem(z_me + r, nz) * nx + x_me)

    def gx_copy(h, r, slot):
        here = gat.at[h, x_me]
        there = gat.at[h, slot]
        return kv_copy(here, there, gx_s.at[h, r - 1], gx_r.at[h, r - 1], z_me * nx + lax.rem(x_me + r, nx))

    wab = jnp.concatenate([wd_v[...], wb_v[...], jnp.zeros((axs.shape[3] - 2 * nheads, width), bf16)], axis=0)
    for r in range(nx):
        rows = nb[:, lax.rem(x_me + r, nx)].reshape(nz * rs, width)
        got = fast_dot(rows, wab, ((1,), (1,))).reshape(nz, rs, -1)
        if r == 0:
            aown[...] = got
        else:
            axs[r - 1] = got.astype(bf16)
            ax_copy(r).start()

    @pl.loop(0, heads)
    def project(h):
        for r in list(range(1, nx)) + [0]:
            rows = nb[:, lax.rem(x_me + r, nx)].reshape(nz * rs, width)
            for i in range(4):
                got = fast_dot(rows, w_v[i, :, lanes(h)]).reshape(nz, rs, dk)
                at = slice(i * dk, (i + 1) * dk)
                if r == 0:
                    own[h, :, :, at] = got
                else:
                    xs[h, r - 1, :, :, at] = got.astype(bf16)
            if r > 0:
                x_copy(h, r).start()

    for r in range(1, nx):
        ax_copy(r).wait_recv()
        aown[...] += axr[r - 1].astype(f32)
    azs[...] = aown[...].astype(bf16)
    for r in range(1, nz):
        az_copy(r).start()

    late[0].wait()

    def stage_b(h):
        for r in range(1, nx):
            x_copy(h, r).wait_recv()
        pair = own[h]
        for r in range(1, nx):
            pair = pair + xr[h, r - 1].astype(f32)
        zs[h] = pair.astype(bf16)
        own[h] = pair
        for r in range(1, nz):
            z_copy(h, r).start()

    def stage_c(h):
        for r in range(1, nz):
            z_copy(h, r).wait_recv()
        tot = own[h, z_me]
        for r in range(1, nz):
            tot = tot + zr[h, r - 1].astype(f32)
        qraw, kraw, vraw, zraw = (tot[:, i * dk : (i + 1) * dk] for i in range(4))

        def unit(v):
            v = v * jax.nn.sigmoid(v)
            return v * lax.rsqrt(jnp.sum(v * v, axis=1, keepdims=True) + epsilon)

        query = unit(qraw) * dk ** (-0.5)
        key = unit(kraw)
        value = vraw * jax.nn.sigmoid(vraw)
        ab = abt[...]
        lane = lax.broadcasted_iota(jnp.int32, ab.shape, 1)
        head = tp * heads + h
        araw = jnp.sum(jnp.where(lane == head, ab, 0.0), axis=1, keepdims=True)
        braw = jnp.sum(jnp.where(lane == head + nheads, ab, 0.0), axis=1, keepdims=True)
        rate_lane = lax.broadcasted_iota(jnp.int32, rate_ref.shape, 1)
        rate = jnp.sum(jnp.where(rate_lane == head, rate_ref[...], 0.0), axis=1, keepdims=True)
        beta = jax.nn.sigmoid(braw)
        softplus = jnp.maximum(araw, 0.0) + jnp.log(1.0 + jnp.exp(-jnp.abs(araw)))
        g = -rate * softplus
        cum, decay, _, strict = chain(g, beta, key, props)
        x = jnp.concatenate([key, query], axis=0)
        prods = split_dot(x, key, ((1,), (1,)))
        a = jnp.where(strict, beta * decay * prods[:rs], 0.0)
        xh, xl = split(x)
        st = car_v[:, h].reshape(seqs * dk, -1)
        sh, sl = split(st)
        wide = spread_rows(xh, seqs, props)
        seen = fast_dot(wide, sh) + (fast_dot(spread_rows(xl, seqs, props), sh) + fast_dot(wide, sl))
        grow = jnp.exp(cum)
        reads = decay * prods[rs:]
        reads = reads - split_dot(reads, a)
        power, reach = a, 2
        while reach < props:
            power = split_dot(power, power)
            reads = reads + split_dot(reads, power)
            reach *= 2
        att = grow * seen[rs:] + split_dot(reads, beta * (value - grow * seen[:rs]))
        ho = att * lax.rsqrt(jnp.mean(att * att, axis=1, keepdims=True) + epsilon)
        ho = ho * hgain_ref[...] * (zraw * jax.nn.sigmoid(zraw))
        gat[h, x_me, z_me] = ho.astype(bf16)
        for r in range(1, nz):
            gz_copy(h, r, z_me).start()

    def stage_d(h):
        for r in range(1, nz):
            gz_copy(h, r, lax.rem(z_me - r + nz, nz)).wait_recv()
        for r in range(1, nx):
            gx_copy(h, r, x_me).start()

    lag_c, lag_d = 2, 4
    stage_b(0)
    for r in range(1, nz):
        az_copy(r).wait_recv()
    ab_total = aown[z_me]
    for r in range(1, nz):
        ab_total = ab_total + azr[r - 1].astype(f32)
    abt[...] = ab_total

    @pl.loop(1, heads + lag_d)
    def pipeline(i):
        @pl.when(i < heads)
        def _():
            stage_b(i)

        @pl.when((i >= lag_c) & (i < heads + lag_c))
        def _():
            stage_c(i - lag_c)

        @pl.when(i >= lag_d)
        def _():
            stage_d(i - lag_d)

    late[1].wait()

    @pl.loop(0, heads)
    def arrived(h):
        for r in range(1, nx):
            gx_copy(h, r, lax.rem(x_me - r + nx, nx)).wait_recv()

    share = rows_all // ntp

    def t_copy(r):
        to = lax.rem(tp + r, ntp)
        return pltpu.make_async_remote_copy(
            src_ref=ts.at[to], dst_ref=tr.at[r - 1], send_sem=t_s.at[r - 1], recv_sem=t_r.at[r - 1],
            device_id={"tp": to}, device_id_type=MESH,
        )

    left = jnp.concatenate(
        [
            jnp.concatenate([gat[h, d % nx, d // nx] for d in range(nkv)], axis=0)
            for h in range(heads)
        ],
        axis=1,
    )
    got = fast_dot(left, wo_v[...]).reshape(ntp, share, -1)
    terms[...] = got
    ts[...] = got.astype(bf16)
    for r in range(1, ntp):
        t_copy(r).start()
    for r in range(1, ntp):
        t_copy(r).wait_recv()
    result = terms[tp]
    for r in range(1, ntp):
        result = result + tr[r - 1].astype(f32)
    out_ref[...] = result.astype(bf16)

    for r in range(1, nkv):
        ss_copy(r, me).wait_send()
    for r in range(1, nx):
        ax_copy(r).wait_send()
    for r in range(1, nz):
        az_copy(r).wait_send()
    for r in range(1, ntp):
        t_copy(r).wait_send()

    @pl.loop(0, heads)
    def drain(h):
        for r in range(1, nx):
            x_copy(h, r).wait_send()
            gx_copy(h, r, x_me).wait_send()
        for r in range(1, nz):
            z_copy(h, r).wait_send()
            gz_copy(h, r, z_me).wait_send()


def step_call(nkv, ntp, tokens, norm_gain, wd, wb, rate, hgain, wq, wk, wv, wz, wo, carried):
    nx = 1
    while nx * nx * 4 <= nkv:
        nx *= 2
    nz = nkv // nx
    seqs, heads, dk, dv = carried.shape
    seqs_all, props, width = tokens.shape
    rs = seqs * props
    rows_all = seqs_all * props
    nheads = wd.shape[0]
    ab = -(-2 * nheads // 128) * 128
    out_cols = wo.shape[1]
    share = rows_all // ntp
    vmem = pl.BlockSpec(memory_space=pltpu.VMEM)
    anyw = pl.BlockSpec(memory_space=pltpu.HBM)
    V = pltpu.VMEM
    dma = pltpu.SemaphoreType.DMA
    return pl.pallas_call(
        functools.partial(step_kernel, nx, nz, ntp),
        out_shape=jax.ShapeDtypeStruct((share, out_cols), bf16),
        in_specs=[vmem, vmem, anyw, anyw, vmem, vmem] + [anyw] * 6,
        out_specs=vmem,
        scratch_shapes=[
            V((rows_all, width), f32),
            V((4,) + wq.shape, bf16),
            V(wo.shape, bf16),
            V((nheads, width), bf16),
            V((nheads, width), bf16),
            V(carried.shape, f32),
            V((nkv, nkv, 128), f32),
            V((nz, nx, rs, width), bf16),
            V((heads, nx - 1, nz, rs, 4 * dk), bf16),
            V((heads, nx - 1, nz, rs, 4 * dk), bf16),
            V((heads, nz, rs, 4 * dk), f32),
            V((heads, nz, rs, 4 * dk), bf16),
            V((heads, nz - 1, rs, 4 * dk), bf16),
            V((nx - 1, nz, rs, ab), bf16),
            V((nx - 1, nz, rs, ab), bf16),
            V((nz, rs, ab), f32),
            V((nz, rs, ab), bf16),
            V((nz - 1, rs, ab), bf16),
            V((rs, ab), f32),
            V((heads, nx, nz, rs, dv), bf16),
            V((ntp, share, out_cols), f32),
            V((ntp, share, out_cols), bf16),
            V((ntp - 1, share, out_cols), bf16),
            dma((8,)),
            dma((nkv - 1,)), dma((nkv - 1,)),
            dma((heads + 1, nx - 1)), dma((heads + 1, nx - 1)),
            dma((heads + 1, nz - 1)), dma((heads + 1, nz - 1)),
            dma((heads, nz - 1)), dma((heads, nz - 1)),
            dma((heads, nx - 1)), dma((heads, nx - 1)),
            dma((ntp - 1,)), dma((ntp - 1,)),
        ],
        compiler_params=pltpu.CompilerParams(
            collective_id=0, has_side_effects=True, vmem_limit_bytes=62 * 1024 * 1024
        ),
    )(tokens, norm_gain, wd, wb, rate, hgain, wq, wk, wv, wz, wo, carried)


def solution(mesh):
    nkv, ntp = mesh.shape["kv"], mesh.shape["tp"]

    def per_device(
        tokens, norm_gain, w_query, w_key, w_value, w_gate, w_decay, w_beta, decay_rate, head_gain, w_out,
        state, prev_keys, prev_values, prev_log_decay, prev_beta, accepted,
    ):
        carried = carried_call(
            state, prev_keys, prev_values, prev_log_decay.transpose(0, 2, 1), prev_beta.transpose(0, 2, 1), accepted
        )
        mixed = step_call(
            nkv, ntp, tokens, norm_gain.reshape(1, -1), w_decay.T, w_beta.T, decay_rate.reshape(1, -1),
            head_gain.reshape(1, -1), w_query, w_key, w_value, w_gate, w_out, carried,
        )
        return mixed.reshape(-1, tokens.shape[1], mixed.shape[1]), carried

    placed = (
        P(None, None, "kv"), P(), P("kv", "tp"), P("kv", "tp"), P("kv", "tp"), P("kv", "tp"), P(), P(), P(), P(),
        P("tp", "kv"), P("kv", "tp", None, None), P("kv", "tp", None, None), P("kv", "tp", None, None),
        P("kv", "tp", None), P("kv", "tp", None), P("kv"),
    )
    return jax.shard_map(
        per_device,
        mesh=mesh,
        in_specs=placed,
        out_specs=(P("tp", None, "kv"), P("kv", "tp", None, None)),
        check_vma=False,
    )
```
